32 devices in a mesh: ep: 8 (over z, x), tp: 4 (over y, core).
Axes of the slice: x: 2, y: 2, z: 4, core: 2. Of those that a mesh axis runs over, the one named last changes fastest.
Arguments:
- stream: bfloat16 [2048, 3072], P('ep'), may hold values from -30 to 30
- ffn_gain: bfloat16 [3072], replicated, may hold values from 0.099609375 to 1.8984375
- chosen: int32 [8, 256], replicated, may hold values from 0 to 2047, as said below
- affinity: float32 [8, 256], P('ep'), may hold values from 0.5 to 2
- w_gate: bfloat16 [8, 3072, 3072], P('ep', None, 'tp'), may hold values from -0.109375 to 0.109375
- w_up: bfloat16 [8, 3072, 3072], P('ep', None, 'tp'), may hold values from -0.109375 to 0.109375
- w_down: bfloat16 [8, 3072, 3072], P('ep', 'tp'), may hold values from -0.109375 to 0.109375
- final_gain: bfloat16 [3072], P('tp'), may hold values from 0.099609375 to 1.8984375
Outputs:
- normed: bfloat16 [2048, 3072], P('ep', 'tp')
The draws below stay inside these ranges and needn't reach their ends.
Inputs may be any that keep to these rules, and one draw needn't show every extreme that they name: `chosen`: row e holds 256 distinct token numbers in ascending order. Of the 256 tokens of one index of ep, each expert reads at least one and at most 48; in every draw some expert reads exactly 48 from some index.
All inputs are finite; a program needn't handle non-finite values.
Results may differ from the reference program's by a relative error of at most 0.015.
Values may be sent and summed in bfloat16 or wider, within the bound.
A program may use at most 128 MiB of HBM per device.

```python
import math
import jax
import jax.numpy as jnp
from jax import lax

D = 3072
FF = 3072
TOK_DEV = 256
TOKENS = 2048
EXPERTS = 8
CAP = 256
N_EP = 8
N_TP = 4


def draw_stream(key, part):
    key_base, key_rows, key_cols = jax.random.split(key, 3)
    ramp = jnp.arange(D, dtype=jnp.float32) / D
    columns = jnp.exp(math.log(0.6) + ramp * math.log(3.0)) * jnp.exp(jax.random.uniform(key_cols, (D,), jnp.float32, -0.3, 0.3))
    base = jnp.clip(jax.random.normal(key_base, (TOKENS, D), jnp.float32), -4.0, 4.0)
    rows_scale = jnp.exp(jax.random.uniform(key_rows, (TOKENS, 1), jnp.float32, math.log(0.3), math.log(3.0)))
    return (base * rows_scale * columns[None, :]).astype(jnp.bfloat16)


def draw_chosen(key, part):
    mean_count = TOK_DEV // 8
    spread = TOK_DEV // 16
    pairs = N_EP // 2
    key_diff, key_pick, key_sign, key_score = jax.random.split(key, 4)
    diff = jax.random.randint(key_diff, (EXPERTS, pairs), -spread, spread + 1)
    forced = jax.random.randint(key_pick, (EXPERTS,), 0, pairs)
    signs = jax.random.randint(key_sign, (EXPERTS,), 0, 2) * 2 - 1
    diff = jnp.where(jnp.arange(pairs)[None, :] == forced[:, None], signs[:, None] * spread, diff)
    counts = jnp.stack([mean_count + diff, mean_count - diff], axis=2).reshape(EXPERTS, N_EP)
    scores = jax.random.randint(key_score, (EXPERTS, N_EP, TOK_DEV), 0, 65536) * TOK_DEV + jnp.arange(TOK_DEV)[None, None, :]
    ranks = jnp.argsort(jnp.argsort(scores, axis=-1), axis=-1)
    selected = (ranks < counts[:, :, None]).reshape(EXPERTS, TOKENS)
    positions = jnp.arange(TOKENS, dtype=jnp.int32)[None, :]
    keyed = jnp.where(selected, positions, positions + TOKENS)
    return jnp.sort(keyed, axis=-1)[:, :CAP].astype(jnp.int32)


def block_scale(own_key, shape, cuts, smallest, high):
    gain = 1.0
    for position, shards_of in cuts:
        steps = jax.random.uniform(jax.random.fold_in(jax.random.fold_in(own_key, 6), position), (shards_of,), jnp.float32, smallest / len(cuts), high / len(cuts))
        gain = gain * jnp.repeat(jnp.exp(steps), shape[position] // shards_of).reshape((-1,) + (1,) * (len(shape) - 1 - position))
    return gain


def centred(own_key, dims, scale, bound, shards=(), kind=jnp.bfloat16):
    values = jax.random.normal(own_key, dims, jnp.float32) * scale
    if len(shards) > 0:
        values = block_scale(own_key, dims, shards, -0.22, 0.18) * values
    return jnp.clip(values, min=-bound, max=bound).astype(kind)


def setup_inputs(seed: int = 0) -> dict:
    key_of = jax.random.split(jax.random.key(seed), 9)
    stream = draw_stream(jax.random.fold_in(key_of[8], 71), 0)
    ffn_gain = jnp.clip(1.0 + 0.18 * jax.random.normal(key_of[1], (D,), jnp.float32), 0.099609375, 1.8984375).astype(jnp.bfloat16)
    chosen = draw_chosen(jax.random.fold_in(key_of[8], 71), 0)
    affinity = jnp.clip(jnp.exp(math.log(2.0) - 1.3862944 * jax.random.uniform(key_of[3], (EXPERTS, CAP), jnp.float32) ** block_scale(key_of[3], (EXPERTS, CAP), ((0, 8),), -0.2, 0.2)), 0.5, 2.0)
    w_gate = centred(key_of[4], (EXPERTS, D, FF), D ** -0.5, 0.109375, ((0, 8), (2, 4)))
    w_up = centred(key_of[5], (EXPERTS, D, FF), D ** -0.5, 0.109375, ((0, 8), (2, 4)))
    w_down = centred(key_of[6], (EXPERTS, FF, D), FF ** -0.5, 0.109375, ((0, 8), (1, 4)))
    final_gain = jnp.clip(1.0 + 0.18 * jax.random.normal(key_of[7], (D,), jnp.float32), 0.099609375, 1.8984375).astype(jnp.bfloat16)
    return dict(stream=stream, ffn_gain=ffn_gain, chosen=chosen, affinity=affinity, w_gate=w_gate, w_up=w_up, w_down=w_down, final_gain=final_gain)


EPSILON = 1e-06

def reference(stream, ffn_gain, chosen, affinity, w_gate, w_up, w_down, final_gain):
    widened = stream.astype(jnp.float32)
    scale_in = lax.rsqrt(lax.optimization_barrier(jnp.mean(widened * widened, axis=-1, keepdims=True)) + EPSILON)
    normed_in = (widened * scale_in * ffn_gain.astype(jnp.float32)).astype(jnp.bfloat16)
    block = FF // N_TP

    def one_expert(update, items):
        token_ids, weights, gate_rows, up_rows, down_rows = items
        picked = normed_in[token_ids]
        gate = jnp.dot(picked, gate_rows, preferred_element_type=jnp.float32)
        up = jnp.dot(picked, up_rows, preferred_element_type=jnp.float32)
        hidden = (jax.nn.silu(gate) * up).astype(jnp.bfloat16)
        blocks = hidden.reshape(CAP, N_TP, block).astype(jnp.float32)
        down_blocks = down_rows.reshape(N_TP, block, D).astype(jnp.float32)
        partial_value = jnp.einsum('cjf,jfd->jcd', blocks, down_blocks).astype(jnp.bfloat16)
        summed = lax.optimization_barrier(jnp.sum(partial_value.astype(jnp.float32), axis=0))
        result = (summed * weights[:, None]).astype(jnp.bfloat16)
        return (update.at[token_ids].add(result.astype(jnp.float32)), None)
    update, unused = lax.scan(one_expert, jnp.zeros((TOKENS, D), jnp.float32), (chosen, affinity, w_gate, w_up, w_down))
    merged = widened + update
    scale_out = lax.rsqrt(lax.optimization_barrier(jnp.mean(merged * merged, axis=-1, keepdims=True)) + EPSILON)
    return (merged * scale_out * final_gain.astype(jnp.float32)).astype(jnp.bfloat16)
```

```python
import functools

import jax
import jax.numpy as jnp
from jax import lax
from jax.experimental import pallas as pl
from jax.experimental.pallas import tpu as pltpu
from jax.sharding import PartitionSpec as P

EPSILON = 1e-06
F32 = jnp.float32
BF16 = jnp.bfloat16
MESH = pl.DeviceIdType.MESH


def layer(
    experts, tp, chunks, slots,
    stream_hbm, gain_ref, chosen_ref, aff_ref, wg_hbm, wu_hbm, wd_hbm, fgain_ref,
    out_ref,
    x_v, xn_v, wg_v, wu_v, wd_v, sel_v, place_v, pack_v, spread_v, aff_v,
    send_v, recv_v, piece_v, accg_v, accu_v, hidden_v,
    psend_v, pown_v, prec_v, ysend_v, yrec_v, leave_v, ret_v, merged_v, ssq_v,
    x_sem, w_sem, wd_sem,
    dsend, drecv, gsend, grecv, fsend, frecv, psend, precv, ysend, yrecv,
    rsend, rrecv, qsend, qrecv,
):
    me = lax.axis_index("ep")
    col = lax.axis_index("tp")
    tok = x_v.shape[0]
    width = x_v.shape[1]
    share = xn_v.shape[1]
    caps = chosen_ref.shape[1]
    cw = share // chunks
    rows = experts * slots
    chips = tp // 2
    y = col // 2
    core = col % 2
    partner = y * 2 + 1 - core

    barrier = pltpu.get_barrier_semaphore()
    for r in range(1, experts):
        pl.semaphore_signal(barrier, inc=1, device_id={"ep": (me + r) % experts}, device_id_type=MESH)
    for r in range(1, tp):
        pl.semaphore_signal(barrier, inc=1, device_id={"tp": (col + r) % tp}, device_id_type=MESH)

    x_copy = pltpu.make_async_copy(stream_hbm, x_v, x_sem)
    x_copy.start()
    w_copies = []
    for k in range(chunks):
        group = []
        for n, (src, dst) in enumerate(((wg_hbm, wg_v), (wu_hbm, wu_v))):
            for j in range(tp):
                copy = pltpu.make_async_copy(
                    src.at[pl.ds(j * share + k * cw, cw), :],
                    dst.at[k, pl.ds(j * cw, cw), :],
                    w_sem.at[k, n, j],
                )
                copy.start()
                group.append(copy)
        w_copies.append(group)
    wd_copy = pltpu.make_async_copy(wd_hbm, wd_v, wd_sem)
    wd_copy.start()

    base = (me * tok).astype(F32)
    lane_cap = lax.broadcasted_iota(jnp.int32, (slots, caps), 1).astype(F32)
    sub_slot = lax.broadcasted_iota(jnp.int32, (slots, caps), 0).astype(F32)
    lane_tok = lax.broadcasted_iota(jnp.int32, (slots, tok), 1).astype(F32)

    def build_sel(e, carry):
        row = chosen_ref[pl.ds(e, 1), :].astype(F32)
        start = jnp.sum(jnp.where(row < base, 1.0, 0.0), axis=1, keepdims=True)
        hit = lane_cap == sub_slot + start
        token = jnp.sum(jnp.where(hit, row + 1.0, 0.0), axis=1, keepdims=True) - 1.0 - base
        sel_v[e] = jnp.where(token == lane_tok, 1.0, 0.0).astype(BF16)
        return carry

    lax.fori_loop(0, experts, build_sel, 0)

    x_copy.wait()
    gain = gain_ref[:, pl.ds(pl.multiple_of(col * share, 128), share)]
    step_rows = 16

    def norm_rows(i, carry):
        at = pl.ds(pl.multiple_of(i * step_rows, step_rows), step_rows)
        block = x_v[at, :].astype(F32)
        scale = lax.rsqrt(jnp.sum(block * block, axis=1, keepdims=True) / width + EPSILON)
        own = x_v[at, pl.ds(pl.multiple_of(col * share, 128), share)].astype(F32)
        xn_v[at, :] = (own * scale * gain).astype(BF16)
        return carry

    lax.fori_loop(0, tok // step_rows, norm_rows, 0)

    pl.semaphore_wait(barrier, experts - 1 + tp - 1)

    sel = sel_v[...].reshape(rows, tok)
    finish = []

    def exchange(k, src, dst, ssem, rsem):
        for r in range(1, experts):
            to = (me + r) % experts
            copy = pltpu.make_async_remote_copy(
                src_ref=src.at[k, to], dst_ref=dst.at[k, me],
                send_sem=ssem.at[k, r], recv_sem=rsem.at[k, r],
                device_id={"ep": to}, device_id_type=MESH,
            )
            copy.start()
            finish.append(copy)
        dst[k, me] = src[k, me]

    def exchange_wait(k, src, dst, ssem, rsem):
        for r in range(1, experts):
            frm = (me + experts - r) % experts
            pltpu.make_async_remote_copy(
                src_ref=src.at[k, me], dst_ref=dst.at[k, frm],
                send_sem=ssem.at[k, r], recv_sem=rsem.at[k, r],
                device_id={"ep": frm}, device_id_type=MESH,
            ).wait_recv()

    for k in range(chunks):
        out = jnp.dot(sel, xn_v[:, k * cw:(k + 1) * cw], preferred_element_type=F32)
        send_v[k] = out.astype(BF16).reshape(experts, slots, cw)
        exchange(k, send_v, recv_v, dsend, drecv)

    own_row = chosen_ref[pl.ds(me, 1), :].astype(F32)
    lane_j = lax.broadcasted_iota(jnp.int32, (1, rows), 1).astype(F32)
    start_j = jnp.zeros((1, rows), F32)
    end_j = jnp.zeros((1, rows), F32)
    slot_j = lane_j
    start_d = jnp.zeros((1, 1), F32)
    for d in range(experts):
        end_d = jnp.sum(jnp.where(own_row < float((d + 1) * tok), 1.0, 0.0), axis=1, keepdims=True)
        mine = (lane_j >= float(d * slots)) & (lane_j < float((d + 1) * slots))
        start_j = start_j + jnp.where(mine, start_d, 0.0)
        end_j = end_j + jnp.where(mine, end_d, 0.0)
        slot_j = slot_j - jnp.where(mine, float(d * slots), 0.0)
        spread_v[d] = jnp.where(
            (lane_cap == sub_slot + start_d) & (lane_cap < end_d), 1.0, 0.0
        ).astype(BF16)
        start_d = end_d
    want = start_j + slot_j
    part = 32

    def build_pack(i, carry):
        at = pl.multiple_of(i * part, part)
        pick = (lax.broadcasted_iota(jnp.int32, (part, rows), 0) + at).astype(F32)
        pack_v[pl.ds(at, part), :] = jnp.where((pick == want) & (pick < end_j), 1.0, 0.0).astype(BF16)
        return carry

    lax.fori_loop(0, caps // part, build_pack, 0)

    square = 128
    eye = (
        lax.broadcasted_iota(jnp.int32, (square, square), 0)
        == lax.broadcasted_iota(jnp.int32, (square, square), 1)
    )
    for b in range(caps // square):
        weights = aff_ref[:, b * square:(b + 1) * square]
        aff_v[b * square:(b + 1) * square, :] = jnp.sum(
            jnp.where(eye, weights, 0.0), axis=1, keepdims=True
        )
    for b in range(rows // square):
        block = sel.astype(F32)[b * square:(b + 1) * square, :]
        place_v[:, b * square:(b + 1) * square] = block.T.astype(BF16)

    def part_of(k, j):
        return piece_v.at[k, :, pl.ds(pl.multiple_of(j * cw, 128), cw)]

    def gather_start(k):
        exchange_wait(k, send_v, recv_v, dsend, drecv)
        got = recv_v[k].reshape(rows, cw)
        own = jnp.dot(pack_v[...], got, preferred_element_type=F32).astype(BF16)
        piece_v[k, :, pl.ds(pl.multiple_of(col * cw, 128), cw)] = own
        for r in range(1, chips):
            to = ((y + r) % chips) * 2 + core
            copy = pltpu.make_async_remote_copy(
                src_ref=part_of(k, col), dst_ref=part_of(k, col),
                send_sem=gsend.at[k, r], recv_sem=grecv.at[k, r],
                device_id={"tp": to}, device_id_type=MESH,
            )
            copy.start()
            finish.append(copy)
        copy = pltpu.make_async_remote_copy(
            src_ref=part_of(k, col), dst_ref=part_of(k, col),
            send_sem=fsend.at[k, 0], recv_sem=frecv.at[k, 0],
            device_id={"tp": partner}, device_id_type=MESH,
        )
        copy.start()
        finish.append(copy)

    def gather_finish(k):
        for r in range(1, chips):
            frm = ((y + chips - r) % chips) * 2 + core
            pltpu.make_async_remote_copy(
                src_ref=part_of(k, col), dst_ref=part_of(k, frm),
                send_sem=gsend.at[k, r], recv_sem=grecv.at[k, r],
                device_id={"tp": frm}, device_id_type=MESH,
            ).wait_recv()
            copy = pltpu.make_async_remote_copy(
                src_ref=part_of(k, frm), dst_ref=part_of(k, frm),
                send_sem=fsend.at[k, r], recv_sem=frecv.at[k, r],
                device_id={"tp": partner}, device_id_type=MESH,
            )
            copy.start()
            finish.append(copy)
        for copy in w_copies[k]:
            copy.wait()
        for r in range(chips):
            theirs = ((y + chips - r) % chips) * 2 + 1 - core
            pltpu.make_async_remote_copy(
                src_ref=part_of(k, col), dst_ref=part_of(k, theirs),
                send_sem=fsend.at[k, r], recv_sem=frecv.at[k, r],
                device_id={"tp": partner}, device_id_type=MESH,
            ).wait_recv()
        taken = piece_v[k]
        gate = jnp.dot(taken, wg_v[k], preferred_element_type=F32)
        accg_v[...] = gate if k == 0 else accg_v[...] + gate
        up = jnp.dot(taken, wu_v[k], preferred_element_type=F32)
        accu_v[...] = up if k == 0 else accu_v[...] + up

    for k in range(chunks):
        gather_start(k)
        if k > 0:
            gather_finish(k - 1)
    gather_finish(chunks - 1)

    hblock = 32

    def activate(i, carry):
        at = pl.ds(pl.multiple_of(i * hblock, hblock), hblock)
        gate = accg_v[at, :]
        hidden_v[at, :] = (gate / (1.0 + jnp.exp(-gate)) * accu_v[at, :]).astype(BF16)
        return carry

    lax.fori_loop(0, caps // hblock, activate, 0)
    wd_copy.wait()

    def down(k, j):
        at = pl.ds(pl.multiple_of(j * share + k * cw, 128), cw)
        return jnp.dot(hidden_v[...], wd_v[:, at], preferred_element_type=F32)

    def pair_copy(k, r):
        return pltpu.make_async_remote_copy(
            src_ref=psend_v.at[k, r], dst_ref=prec_v.at[k, r],
            send_sem=psend.at[k, r], recv_sem=precv.at[k, r],
            device_id={"tp": partner}, device_id_type=MESH,
        )

    order = [r for r in range(1, chips)] + [0]

    def stage_pair(k):
        for r in order:
            to = (y + r) % chips
            psend_v[k, r] = down(k, to * 2 + 1 - core).astype(BF16)
            copy = pair_copy(k, r)
            copy.start()
            finish.append(copy)
        for r in order:
            to = (y + r) % chips
            pown_v[k, r] = down(k, to * 2 + core)

    def chip_copy(k, r):
        to = ((y + r) % chips) * 2 + core
        return pltpu.make_async_remote_copy(
            src_ref=ysend_v.at[k, r], dst_ref=yrec_v.at[k, r],
            send_sem=ysend.at[k, r], recv_sem=yrecv.at[k, r],
            device_id={"tp": to}, device_id_type=MESH,
        )

    def stage_chip(k):
        for r in order:
            pair_copy(k, r).wait_recv()
            both = pown_v[k, r] + prec_v[k, r].astype(F32)
            if r == 0:
                pown_v[k, r] = both
            else:
                ysend_v[k, r] = both.astype(BF16)
                copy = chip_copy(k, r)
                copy.start()
                finish.append(copy)

    def stage_leave(k):
        total = pown_v[k, 0]
        for r in range(1, chips):
            chip_copy(k, r).wait_recv()
            total = total + yrec_v[k, r].astype(F32)
        weighted = (total * aff_v[...]).astype(BF16)
        spread = spread_v[...].reshape(rows, caps)
        out = jnp.dot(spread, weighted, preferred_element_type=F32)
        leave_v[k] = out.astype(BF16).reshape(experts, slots, cw)
        exchange(k, leave_v, ret_v, rsend, rrecv)

    for k in range(chunks):
        stage_pair(k)
        if k > 0:
            stage_chip(k - 1)
    stage_chip(chunks - 1)
    for k in range(chunks):
        stage_leave(k)

    squares = jnp.zeros((tok, 1), F32)
    for k in range(chunks):
        exchange_wait(k, leave_v, ret_v, rsend, rrecv)
        update = jnp.dot(place_v[...], ret_v[k].reshape(rows, cw), preferred_element_type=F32)
        at = pl.ds(pl.multiple_of(col * share + k * cw, 128), cw)
        merged = x_v[:, at].astype(F32) + update
        merged_v[k] = merged
        squares = squares + jnp.sum(merged * merged, axis=1, keepdims=True)

    for b in range(tok // square):
        line = jnp.sum(
            jnp.where(eye, squares[b * square:(b + 1) * square, :], 0.0), axis=0, keepdims=True
        )
        ssq_v[0, :, b * square:(b + 1) * square] = jnp.broadcast_to(line, (8, square))

    def square_copy(r):
        return pltpu.make_async_remote_copy(
            src_ref=ssq_v.at[0], dst_ref=ssq_v.at[r],
            send_sem=qsend.at[r], recv_sem=qrecv.at[r],
            device_id={"tp": (col + r) % tp}, device_id_type=MESH,
        )

    for r in range(1, tp):
        copy = square_copy(r)
        copy.start()
        finish.append(copy)
    sums = ssq_v[0]
    for r in range(1, tp):
        square_copy(r).wait_recv()
        sums = sums + ssq_v[r]
    for b in range(tok // square):
        line = sums[0:1, b * square:(b + 1) * square]
        column = jnp.sum(jnp.where(eye, line, 0.0), axis=1, keepdims=True)
        scale = lax.rsqrt(column / width + EPSILON)
        for k in range(chunks):
            block = merged_v[k, b * square:(b + 1) * square, :]
            out_ref[b * square:(b + 1) * square, k * cw:(k + 1) * cw] = (
                block * scale * fgain_ref[:, k * cw:(k + 1) * cw]
            ).astype(BF16)

    for copy in finish:
        copy.wait_send()


def on_device(stream, ffn_gain, chosen, affinity, w_gate, w_up, w_down, final_gain):
    tok, width = stream.shape
    experts, caps = chosen.shape
    tp = lax.axis_size("tp")
    share = width // tp
    hid = w_gate.shape[2]
    slots = 3 * tok // 16
    chunks = 3 if share % 384 == 0 else 1
    cw = share // chunks
    chips = tp // 2
    rows = experts * slots
    vmem = pl.BlockSpec(memory_space=pltpu.VMEM)
    hbm = pl.BlockSpec(memory_space=pl.ANY)
    dma = pltpu.SemaphoreType.DMA
    return pl.pallas_call(
        functools.partial(layer, experts, tp, chunks, slots),
        out_shape=jax.ShapeDtypeStruct((tok, share), BF16),
        in_specs=[hbm, vmem, vmem, vmem, hbm, hbm, hbm, vmem],
        out_specs=vmem,
        scratch_shapes=[
            pltpu.VMEM((tok, width), BF16),
            pltpu.VMEM((tok, share), BF16),
            pltpu.VMEM((chunks, tp * cw, hid), BF16),
            pltpu.VMEM((chunks, tp * cw, hid), BF16),
            pltpu.VMEM((hid, width), BF16),
            pltpu.VMEM((experts, slots, tok), BF16),
            pltpu.VMEM((tok, rows), BF16),
            pltpu.VMEM((caps, rows), BF16),
            pltpu.VMEM((experts, slots, caps), BF16),
            pltpu.VMEM((caps, 1), F32),
            pltpu.VMEM((chunks, experts, slots, cw), BF16),
            pltpu.VMEM((chunks, experts, slots, cw), BF16),
            pltpu.VMEM((chunks, caps, tp * cw), BF16),
            pltpu.VMEM((caps, hid), F32),
            pltpu.VMEM((caps, hid), F32),
            pltpu.VMEM((caps, hid), BF16),
            pltpu.VMEM((chunks, chips, caps, cw), BF16),
            pltpu.VMEM((chunks, chips, caps, cw), F32),
            pltpu.VMEM((chunks, chips, caps, cw), BF16),
            pltpu.VMEM((chunks, chips, caps, cw), BF16),
            pltpu.VMEM((chunks, chips, caps, cw), BF16),
            pltpu.VMEM((chunks, experts, slots, cw), BF16),
            pltpu.VMEM((chunks, experts, slots, cw), BF16),
            pltpu.VMEM((chunks, tok, cw), F32),
            pltpu.VMEM((tp, 8, tok), F32),
            dma, dma((chunks, 2, tp)), dma,
            dma((chunks, experts)), dma((chunks, experts)),
            dma((chunks, chips)), dma((chunks, chips)),
            dma((chunks, chips)), dma((chunks, chips)),
            dma((chunks, chips)), dma((chunks, chips)),
            dma((chunks, chips)), dma((chunks, chips)),
            dma((chunks, experts)), dma((chunks, experts)),
            dma((tp,)), dma((tp,)),
        ],
        compiler_params=pltpu.CompilerParams(
            collective_id=0, has_side_effects=True, vmem_limit_bytes=60 * 1024 * 1024
        ),
        name="layer",
    )(
        stream,
        ffn_gain.astype(F32)[None, :],
        chosen,
        affinity,
        w_gate[0],
        w_up[0],
        w_down[0],
        final_gain.astype(F32)[None, :],
    )


def solution(mesh):
    return jax.shard_map(
        on_device,
        mesh=mesh,
        in_specs=(
            P("ep", None),
            P(),
            P(),
            P("ep", None),
            P("ep", None, "tp"),
            P("ep", None, "tp"),
            P("ep", "tp", None),
            P("tp"),
        ),
        out_specs=P("ep", "tp"),
        check_vma=False,
    )
```

```python
import functools

import jax
import jax.numpy as jnp
from jax import lax
from jax.experimental import pallas as pl
from jax.experimental.pallas import tpu as pltpu
from jax.sharding import PartitionSpec as P

EPSILON = 1e-06
F32 = jnp.float32
BF16 = jnp.bfloat16
MESH = pl.DeviceIdType.MESH


def layer(
    experts, tp, chunks, slots,
    stream_hbm, gain_ref, chosen_ref, aff_ref, wg_hbm, wu_hbm, wd_hbm, fgain_ref,
    out_ref,
    x_v, xn_v, wg_v, wu_v, wd_v, sel_v, place_v, pack_v, spread_v, aff_v,
    send_v, recv_v, piece_v, accg_v, accu_v, hidden_v,
    psend_v, pown_v, prec_v, ysend_v, yrec_v, leave_v, ret_v, merged_v, ssq_v, gain_v,
    x_sem, w_sem, wd_sem,
    dsend, drecv, gsend, grecv, fsend, frecv, psend, precv, ysend, yrecv,
    rsend, rrecv, qsend, qrecv,
):
    me = lax.axis_index("ep")
    col = lax.axis_index("tp")
    tok = x_v.shape[0]
    width = x_v.shape[1]
    share = xn_v.shape[1]
    caps = chosen_ref.shape[1]
    cw = share // chunks
    rows = experts * slots
    chips = tp // 2
    y = col // 2
    core = col % 2
    partner = y * 2 + 1 - core

    barrier = pltpu.get_barrier_semaphore()
    for r in range(1, experts):
        pl.semaphore_signal(barrier, inc=1, device_id={"ep": (me + r) % experts}, device_id_type=MESH)
    for r in range(1, tp):
        pl.semaphore_signal(barrier, inc=1, device_id={"tp": (col + r) % tp}, device_id_type=MESH)

    x_copy = pltpu.make_async_copy(stream_hbm, x_v, x_sem)
    x_copy.start()
    w_copies = []
    for k in range(chunks):
        group = []
        for n, (src, dst) in enumerate(((wg_hbm, wg_v), (wu_hbm, wu_v))):
            for j in range(tp):
                copy = pltpu.make_async_copy(
                    src.at[pl.ds(j * share + k * cw, cw), :],
                    dst.at[k, pl.ds(j * cw, cw), :],
                    w_sem.at[k, n, j],
                )
                copy.start()
                group.append(copy)
        w_copies.append(group)
    wd_copy = pltpu.make_async_copy(wd_hbm, wd_v, wd_sem)
    wd_copy.start()

    base = (me * tok).astype(F32)
    lane_cap = lax.broadcasted_iota(jnp.int32, (slots, caps), 1).astype(F32)
    sub_slot = lax.broadcasted_iota(jnp.int32, (slots, caps), 0).astype(F32)
    lane_tok = lax.broadcasted_iota(jnp.int32, (slots, tok), 1).astype(F32)

    def build_sel(e, carry):
        row = chosen_ref[pl.ds(e, 1), :].astype(F32)
        start = jnp.sum(jnp.where(row < base, 1.0, 0.0), axis=1, keepdims=True)
        hit = lane_cap == sub_slot + start
        token = jnp.sum(jnp.where(hit, row + 1.0, 0.0), axis=1, keepdims=True) - 1.0 - base
        sel_v[e] = jnp.where(token == lane_tok, 1.0, 0.0).astype(BF16)
        return carry

    lax.fori_loop(0, experts, build_sel, 0)

    x_copy.wait()
    gain_v[...] = gain_ref[...].astype(F32)
    lines = share // 128
    gain = jnp.concatenate(
        [gain_v[pl.ds(col * lines + i, 1), :] for i in range(lines)], axis=1
    )
    step_rows = 16

    def norm_rows(i, carry):
        at = pl.ds(pl.multiple_of(i * step_rows, step_rows), step_rows)
        block = x_v[at, :].astype(F32)
        scale = lax.rsqrt(jnp.sum(block * block, axis=1, keepdims=True) / width + EPSILON)
        own = x_v[at, pl.ds(pl.multiple_of(col * share, 128), share)].astype(F32)
        xn_v[at, :] = (own * scale * gain).astype(BF16)
        return carry

    lax.fori_loop(0, tok // step_rows, norm_rows, 0)

    sel = sel_v[...].reshape(rows, tok)
    finish = []

    def exchange(k, src, dst, ssem, rsem):
        for r in range(1, experts):
            to = (me + r) % experts
            copy = pltpu.make_async_remote_copy(
                src_ref=src.at[k, to], dst_ref=dst.at[k, me],
                send_sem=ssem.at[k, r], recv_sem=rsem.at[k, r],
                device_id={"ep": to}, device_id_type=MESH,
            )
            copy.start()
            finish.append(copy)
        dst[k, me] = src[k, me]

    def exchange_wait(k, src, dst, ssem, rsem):
        for r in range(1, experts):
            frm = (me + experts - r) % experts
            pltpu.make_async_remote_copy(
                src_ref=src.at[k, me], dst_ref=dst.at[k, frm],
                send_sem=ssem.at[k, r], recv_sem=rsem.at[k, r],
                device_id={"ep": frm}, device_id_type=MESH,
            ).wait_recv()

    for k in range(chunks):
        out = jnp.dot(sel, xn_v[:, k * cw:(k + 1) * cw], preferred_element_type=F32)
        send_v[k] = out.astype(BF16).reshape(experts, slots, cw)
    pl.semaphore_wait(barrier, experts - 1 + tp - 1)
    for k in range(chunks):
        exchange(k, send_v, recv_v, dsend, drecv)

    own_row = chosen_ref[pl.ds(me, 1), :].astype(F32)
    lane_j = lax.broadcasted_iota(jnp.int32, (1, rows), 1).astype(F32)
    start_j = jnp.zeros((1, rows), F32)
    end_j = jnp.zeros((1, rows), F32)
    slot_j = lane_j
    start_d = jnp.zeros((1, 1), F32)
    for d in range(experts):
        end_d = jnp.sum(jnp.where(own_row < float((d + 1) * tok), 1.0, 0.0), axis=1, keepdims=True)
        mine = (lane_j >= float(d * slots)) & (lane_j < float((d + 1) * slots))
        start_j = start_j + jnp.where(mine, start_d, 0.0)
        end_j = end_j + jnp.where(mine, end_d, 0.0)
        slot_j = slot_j - jnp.where(mine, float(d * slots), 0.0)
        spread_v[d] = jnp.where(
            (lane_cap == sub_slot + start_d) & (lane_cap < end_d), 1.0, 0.0
        ).astype(BF16)
        start_d = end_d
    want = start_j + slot_j
    part = 32

    def build_pack(i, carry):
        at = pl.multiple_of(i * part, part)
        pick = (lax.broadcasted_iota(jnp.int32, (part, rows), 0) + at).astype(F32)
        pack_v[pl.ds(at, part), :] = jnp.where((pick == want) & (pick < end_j), 1.0, 0.0).astype(BF16)
        return carry

    lax.fori_loop(0, caps // part, build_pack, 0)

    square = 128
    eye = (
        lax.broadcasted_iota(jnp.int32, (square, square), 0)
        == lax.broadcasted_iota(jnp.int32, (square, square), 1)
    )
    for b in range(caps // square):
        weights = aff_ref[:, b * square:(b + 1) * square]
        aff_v[b * square:(b + 1) * square, :] = jnp.sum(
            jnp.where(eye, weights, 0.0), axis=1, keepdims=True
        )
    for b in range(rows // square):
        block = sel.astype(F32)[b * square:(b + 1) * square, :]
        place_v[:, b * square:(b + 1) * square] = block.T.astype(BF16)

    def part_of(k, j):
        return piece_v.at[k, :, pl.ds(pl.multiple_of(j * cw, 128), cw)]

    def gather_start(k):
        exchange_wait(k, send_v, recv_v, dsend, drecv)
        got = recv_v[k].reshape(rows, cw)
        own = jnp.dot(pack_v[...], got, preferred_element_type=F32).astype(BF16)
        piece_v[k, :, pl.ds(pl.multiple_of(col * cw, 128), cw)] = own
        for r in range(1, chips):
            to = ((y + r) % chips) * 2 + core
            copy = pltpu.make_async_remote_copy(
                src_ref=part_of(k, col), dst_ref=part_of(k, col),
                send_sem=gsend.at[k, r], recv_sem=grecv.at[k, r],
                device_id={"tp": to}, device_id_type=MESH,
            )
            copy.start()
            finish.append(copy)
        copy = pltpu.make_async_remote_copy(
            src_ref=part_of(k, col), dst_ref=part_of(k, col),
            send_sem=fsend.at[k, 0], recv_sem=frecv.at[k, 0],
            device_id={"tp": partner}, device_id_type=MESH,
        )
        copy.start()
        finish.append(copy)

    def gather_finish(k):
        for r in range(1, chips):
            frm = ((y + chips - r) % chips) * 2 + core
            pltpu.make_async_remote_copy(
                src_ref=part_of(k, col), dst_ref=part_of(k, frm),
                send_sem=gsend.at[k, r], recv_sem=grecv.at[k, r],
                device_id={"tp": frm}, device_id_type=MESH,
            ).wait_recv()
            copy = pltpu.make_async_remote_copy(
                src_ref=part_of(k, frm), dst_ref=part_of(k, frm),
                send_sem=fsend.at[k, r], recv_sem=frecv.at[k, r],
                device_id={"tp": partner}, device_id_type=MESH,
            )
            copy.start()
            finish.append(copy)
        for copy in w_copies[k]:
            copy.wait()
        for r in range(chips):
            theirs = ((y + chips - r) % chips) * 2 + 1 - core
            pltpu.make_async_remote_copy(
                src_ref=part_of(k, col), dst_ref=part_of(k, theirs),
                send_sem=fsend.at[k, r], recv_sem=frecv.at[k, r],
                device_id={"tp": partner}, device_id_type=MESH,
            ).wait_recv()
        taken = piece_v[k]
        gate = jnp.dot(taken, wg_v[k], preferred_element_type=F32)
        accg_v[...] = gate if k == 0 else accg_v[...] + gate
        up = jnp.dot(taken, wu_v[k], preferred_element_type=F32)
        accu_v[...] = up if k == 0 else accu_v[...] + up

    for k in range(chunks):
        gather_start(k)
        if k > 0:
            gather_finish(k - 1)
    gather_finish(chunks - 1)

    hblock = 32

    def activate(i, carry):
        at = pl.ds(pl.multiple_of(i * hblock, hblock), hblock)
        gate = accg_v[at, :]
        hidden_v[at, :] = (gate / (1.0 + jnp.exp(-gate)) * accu_v[at, :]).astype(BF16)
        return carry

    lax.fori_loop(0, caps // hblock, activate, 0)
    wd_copy.wait()

    def down(k, j):
        at = pl.ds(pl.multiple_of(j * share + k * cw, 128), cw)
        return jnp.dot(hidden_v[...], wd_v[:, at], preferred_element_type=F32)

    def pair_copy(k, r):
        return pltpu.make_async_remote_copy(
            src_ref=psend_v.at[k, r], dst_ref=prec_v.at[k, r],
            send_sem=psend.at[k, r], recv_sem=precv.at[k, r],
            device_id={"tp": partner}, device_id_type=MESH,
        )

    away = list(range(1, chips))

    def stage_pair(k, turns):
        for r in turns:
            to = (y + r) % chips
            psend_v[k, r] = down(k, to * 2 + 1 - core).astype(BF16)
            copy = pair_copy(k, r)
            copy.start()
            finish.append(copy)
        for r in turns:
            to = (y + r) % chips
            pown_v[k, r] = down(k, to * 2 + core)

    def chip_copy(k, r):
        to = ((y + r) % chips) * 2 + core
        return pltpu.make_async_remote_copy(
            src_ref=ysend_v.at[k, r], dst_ref=yrec_v.at[k, r],
            send_sem=ysend.at[k, r], recv_sem=yrecv.at[k, r],
            device_id={"tp": to}, device_id_type=MESH,
        )

    def stage_chip(k, turns):
        for r in turns:
            pair_copy(k, r).wait_recv()
            both = pown_v[k, r] + prec_v[k, r].astype(F32)
            if r == 0:
                pown_v[k, r] = both
            else:
                ysend_v[k, r] = both.astype(BF16)
                copy = chip_copy(k, r)
                copy.start()
                finish.append(copy)

    def stage_leave(k):
        total = pown_v[k, 0]
        for r in range(1, chips):
            chip_copy(k, r).wait_recv()
            total = total + yrec_v[k, r].astype(F32)
        weighted = (total * aff_v[...]).astype(BF16)
        spread = spread_v[...].reshape(rows, caps)
        out = jnp.dot(spread, weighted, preferred_element_type=F32)
        leave_v[k] = out.astype(BF16).reshape(experts, slots, cw)
        exchange(k, leave_v, ret_v, rsend, rrecv)

    for k in range(chunks):
        stage_pair(k, away)
        if k > 0:
            stage_chip(k - 1, away)
    stage_pair(0, [0])
    stage_chip(chunks - 1, away)
    for k in range(1, chunks):
        stage_pair(k, [0])
    for k in range(chunks):
        stage_chip(k, [0])
        stage_leave(k)

    squares = jnp.zeros((tok, 1), F32)
    for k in range(chunks):
        exchange_wait(k, leave_v, ret_v, rsend, rrecv)
        update = jnp.dot(place_v[...], ret_v[k].reshape(rows, cw), preferred_element_type=F32)
        at = pl.ds(pl.multiple_of(col * share + k * cw, 128), cw)
        merged = x_v[:, at].astype(F32) + update
        merged_v[:, k * cw:(k + 1) * cw] = merged
        squares = squares + jnp.sum(merged * merged, axis=1, keepdims=True)

    for b in range(tok // square):
        line = jnp.sum(
            jnp.where(eye, squares[b * square:(b + 1) * square, :], 0.0), axis=0, keepdims=True
        )
        ssq_v[0, :, b * square:(b + 1) * square] = jnp.broadcast_to(line, (8, square))

    def square_copy(r):
        return pltpu.make_async_remote_copy(
            src_ref=ssq_v.at[0], dst_ref=ssq_v.at[r],
            send_sem=qsend.at[r], recv_sem=qrecv.at[r],
            device_id={"tp": (col + r) % tp}, device_id_type=MESH,
        )

    for r in range(1, tp):
        copy = square_copy(r)
        copy.start()
        finish.append(copy)
    closing = fgain_ref[...].astype(F32)
    fgain = jnp.concatenate([closing[i:i + 1, :] for i in range(lines)], axis=1)
    sums = ssq_v[0]
    for r in range(1, tp):
        square_copy(r).wait_recv()
        sums = sums + ssq_v[r]
    for b in range(tok // square):
        line = sums[0:1, b * square:(b + 1) * square]
        column = jnp.sum(jnp.where(eye, line, 0.0), axis=1, keepdims=True)
        scale = lax.rsqrt(column / width + EPSILON)
        at = slice(b * square, (b + 1) * square)
        out_ref[at, :] = (merged_v[at, :] * scale * fgain).astype(BF16)

    for copy in finish:
        copy.wait_send()


def on_device(stream, ffn_gain, chosen, affinity, w_gate, w_up, w_down, final_gain):
    tok, width = stream.shape
    experts, caps = chosen.shape
    tp = lax.axis_size("tp")
    share = width // tp
    hid = w_gate.shape[2]
    slots = 3 * tok // 16
    chunks = 3 if share % 384 == 0 else 1
    cw = share // chunks
    chips = tp // 2
    rows = experts * slots
    vmem = pl.BlockSpec(memory_space=pltpu.VMEM)
    hbm = pl.BlockSpec(memory_space=pltpu.HBM)
    dma = pltpu.SemaphoreType.DMA
    buffers = [
        pltpu.VMEM((tok, width), BF16),
        pltpu.VMEM((tok, share), BF16),
        pltpu.VMEM((chunks, tp * cw, hid), BF16),
        pltpu.VMEM((chunks, tp * cw, hid), BF16),
        pltpu.VMEM((hid, width), BF16),
        pltpu.VMEM((experts, slots, tok), BF16),
        pltpu.VMEM((tok, rows), BF16),
        pltpu.VMEM((caps, rows), BF16),
        pltpu.VMEM((experts, slots, caps), BF16),
        pltpu.VMEM((caps, 1), F32),
        pltpu.VMEM((chunks, experts, slots, cw), BF16),
        pltpu.VMEM((chunks, experts, slots, cw), BF16),
        pltpu.VMEM((chunks, caps, tp * cw), BF16),
        pltpu.VMEM((caps, hid), F32),
        pltpu.VMEM((caps, hid), F32),
        pltpu.VMEM((caps, hid), BF16),
        pltpu.VMEM((chunks, chips, caps, cw), BF16),
        pltpu.VMEM((chunks, chips, caps, cw), F32),
        pltpu.VMEM((chunks, chips, caps, cw), BF16),
        pltpu.VMEM((chunks, chips, caps, cw), BF16),
        pltpu.VMEM((chunks, chips, caps, cw), BF16),
        pltpu.VMEM((chunks, experts, slots, cw), BF16),
        pltpu.VMEM((chunks, experts, slots, cw), BF16),
        pltpu.VMEM((tok, share), F32),
        pltpu.VMEM((tp, 8, tok), F32),
        pltpu.VMEM((width // 128, 128), F32),
    ]
    return pl.pallas_call(
        functools.partial(layer, experts, tp, chunks, slots),
        out_shape=jax.ShapeDtypeStruct((tok, share), BF16),
        in_specs=[hbm, vmem, vmem, vmem, hbm, hbm, hbm, vmem],
        out_specs=vmem,
        scratch_shapes=buffers + [
            dma, dma((chunks, 2, tp)), dma,
            dma((chunks, experts)), dma((chunks, experts)),
            dma((chunks, chips)), dma((chunks, chips)),
            dma((chunks, chips)), dma((chunks, chips)),
            dma((chunks, chips)), dma((chunks, chips)),
            dma((chunks, chips)), dma((chunks, chips)),
            dma((chunks, experts)), dma((chunks, experts)),
            dma((tp,)), dma((tp,)),
        ],
        compiler_params=pltpu.CompilerParams(
            collective_id=0, has_side_effects=True, vmem_limit_bytes=60 * 1024 * 1024
        ),
        name="layer",
    )(
        stream,
        ffn_gain.reshape(width // 128, 128),
        chosen,
        affinity,
        w_gate[0],
        w_up[0],
        w_down[0],
        final_gain.reshape(share // 128, 128),
    )


def solution(mesh):
    return jax.shard_map(
        on_device,
        mesh=mesh,
        in_specs=(
            P("ep", None),
            P(),
            P(),
            P("ep", None),
            P("ep", None, "tp"),
            P("ep", None, "tp"),
            P("ep", "tp", None),
            P("tp"),
        ),
        out_specs=P("ep", "tp"),
        check_vma=False,
    )
```
